32 devices in a mesh: sp: 16 (over z, y, core), tp: 2 (over x).
Axes of the slice: x: 2, y: 2, z: 4, core: 2. Of those that a mesh axis runs over, the one named last changes fastest.
Arguments:
- inputs: bfloat16 [2, 2048, 1024], P(None, 'sp'), may hold values from -6 to 6
- queries: bfloat16 [2, 2048, 4, 128], P(None, 'sp', 'tp'), may hold values from -6 to 6
- values: bfloat16 [2, 2048, 4, 256], P(None, 'sp', 'tp'), may hold values from -6 to 6
- out_grad: bfloat16 [2, 2048, 4, 256], P(None, 'sp', 'tp'), may hold values from -6 to 6
- key_weight: bfloat16 [1024, 4, 128], P(None, 'tp'), may hold values from -6 to 6
- decay_ahead: float32 [4], P('tp'), may hold values from -2.9 to 2.2
- decay_behind: float32 [4], P('tp'), may hold values from -2.9 to 2.2
Outputs:
- query_grad: bfloat16 [2, 2048, 4, 128], P(None, 'sp', 'tp')
- value_grad: bfloat16 [2, 2048, 4, 256], P(None, 'sp', 'tp')
- input_grad: bfloat16 [2, 2048, 1024], P('tp', 'sp')
- weight_grad: float32 [1024, 4, 128], P('sp', 'tp')
- decay_grad: float32 [2, 4], P(None, 'tp')
The draws below stay inside these ranges and needn't reach their ends.
All inputs are finite; a program needn't handle non-finite values.
Results may differ from the reference program's by a relative error of at most 0.015.
Values may be sent and summed in bfloat16 or wider, within the bound.
A program may use at most 256 MiB of HBM per device.

```python
import math
import jax
import jax.numpy as jnp
from jax import lax

D = 1024
HEADS = 4
DK = 128
DV = 256
SEQS = 2
TOK_DEV = 128
TOKENS = 2048


def strengthened(drawn, rng, source, target, parts, factor):
    owner, partner = [(jnp.arange(drawn.shape[axis_at]) // (drawn.shape[axis_at] // parts)).reshape([-1 if axis == axis_at else 1 for axis in range(drawn.ndim)]) for axis_at in (source, target)]
    chosen = jax.random.permutation(rng, parts)[partner]
    strong = (owner == chosen) | (owner == (partner + parts // 2) % parts)
    return jnp.where(strong, factor * drawn, drawn)


def level_of(own_key, extent, pieces, smallest, top_value):
    def one(axis_at, shards_of):
        steps = jax.random.uniform(jax.random.fold_in(jax.random.fold_in(own_key, 6), axis_at), (shards_of,), jnp.float32, smallest / len(pieces), top_value / len(pieces))
        return jnp.repeat(jnp.exp(steps), extent[axis_at] // shards_of).reshape((-1,) + (1,) * (len(extent) - axis_at - 1))

    level = one(*pieces[0])
    for cut in pieces[1:]:
        level = level * one(*cut)
    return level


def scatter_about(key, shape, deviation, most, pieces=(), kind=jnp.bfloat16):
    drawn = jax.random.normal(key, shape, jnp.float32) * deviation
    if len(pieces) > 0:
        drawn = level_of(key, shape, pieces, -0.22, 0.18) * drawn
    return jnp.clip(drawn, min=-most, max=most).astype(kind)


def bell_draw_with(own_key, dims, deviation, bound, pieces, heavy, kind=jnp.bfloat16):
    array = deviation * jax.random.normal(own_key, dims, jnp.float32)
    if pieces:
        array = array * level_of(own_key, dims, pieces, -0.22, 0.18)
    return jnp.clip(strengthened(array, jax.random.fold_in(own_key, 3), *heavy), -bound, bound).astype(kind)


def setup_inputs(seed: int = 0) -> dict:
    streams_of = jax.random.split(jax.random.key(seed), 8)
    inputs = bell_draw_with(streams_of[0], (SEQS, TOKENS, D), 1.0, 6.0, ((1, 16),), (1, 2, 16, 2.0))
    queries = scatter_about(streams_of[1], (SEQS, TOKENS, HEADS, DK), 1.0, 6.0, ((1, 16), (2, 2)))
    values = scatter_about(streams_of[2], (SEQS, TOKENS, HEADS, DV), 1.0, 6.0, ((1, 16), (2, 2)))
    out_grad = scatter_about(streams_of[3], (SEQS, TOKENS, HEADS, DV), 1.0, 6.0, ((1, 16), (2, 2)))
    key_weight = scatter_about(streams_of[4], (D, HEADS, DK), 1.0, 6.0, ((1, 2),))
    decay_ahead = jnp.clip(-2.9 + 5.1000001430511475 * jax.random.uniform(streams_of[5], (HEADS,), jnp.float32) ** level_of(streams_of[5], (HEADS,), ((0, 2),), -0.2, 0.2), -2.9, 2.2)
    decay_behind = jnp.clip(-2.9 + 5.1000001430511475 * jax.random.uniform(streams_of[6], (HEADS,), jnp.float32) ** level_of(streams_of[6], (HEADS,), ((0, 2),), -0.2, 0.2), -2.9, 2.2)
    return {"inputs": inputs, "queries": queries, "values": values, "out_grad": out_grad, "key_weight": key_weight, "decay_ahead": decay_ahead, "decay_behind": decay_behind}


HIGHEST = lax.Precision.HIGHEST

def retention(queries, keys, values, decay_ahead, decay_behind):
    all_tokens = queries.shape[0]
    blocks = all_tokens // TOK_DEV
    rate_ahead = jax.nn.log_sigmoid(decay_ahead) / all_tokens
    rate_behind = jax.nn.log_sigmoid(decay_behind) / all_tokens
    offsets = jnp.arange(TOK_DEV, dtype=jnp.float32)
    distance = offsets[:, None] - offsets[None, :]
    mask_ahead = jnp.where(distance[None] >= 0, jnp.exp(distance[None] * rate_ahead[:, None, None]), 0.0)
    mask_behind = jnp.where(distance[None] <= 0, jnp.exp(-distance[None] * rate_behind[:, None, None]), 0.0)
    keep_ahead = jnp.exp((TOK_DEV - 1.0 - offsets)[:, None] * rate_ahead[None])
    keep_behind = jnp.exp(offsets[:, None] * rate_behind[None])
    reach_ahead = jnp.exp((offsets + 1.0)[:, None] * rate_ahead[None])
    reach_behind = jnp.exp((TOK_DEV - offsets)[:, None] * rate_behind[None])
    query_blocks = queries.reshape(blocks, TOK_DEV, HEADS, -1)
    key_blocks = keys.reshape(blocks, TOK_DEV, HEADS, -1)
    value_blocks = values.reshape(blocks, TOK_DEV, HEADS, -1)
    scores = jnp.einsum('nthk,nshk->nhts', query_blocks, key_blocks, precision=HIGHEST)
    near = jnp.einsum('nhts,nshv->nthv', scores * (mask_ahead + mask_behind)[None], value_blocks, precision=HIGHEST)
    sums_ahead = jnp.einsum('nshk,nshv->nhkv', key_blocks * keep_ahead[None, :, :, None], value_blocks, precision=HIGHEST)
    sums_behind = jnp.einsum('nshk,nshv->nhkv', key_blocks * keep_behind[None, :, :, None], value_blocks, precision=HIGHEST)
    span_ahead = jnp.exp(TOK_DEV * rate_ahead)[:, None, None]
    span_behind = jnp.exp(TOK_DEV * rate_behind)[:, None, None]
    zero_state = jnp.zeros(sums_ahead.shape[1:], jnp.float32)

    def carry_ahead(state, piece):
        return (span_ahead * state + piece, state)

    def carry_behind(state, piece):
        return (span_behind * state + piece, state)
    _, before = lax.scan(carry_ahead, zero_state, sums_ahead)
    _, after = lax.scan(carry_behind, zero_state, sums_behind, reverse=True)
    far = jnp.einsum('nthk,nhkv->nthv', query_blocks * reach_ahead[None, :, :, None], before, precision=HIGHEST)
    far = far + jnp.einsum('nthk,nhkv->nthv', query_blocks * reach_behind[None, :, :, None], after, precision=HIGHEST)
    return (near + far).reshape(all_tokens, HEADS, -1)

def reference(inputs, queries, values, out_grad, key_weight, decay_ahead, decay_behind):
    key_scale = 1.0 / math.sqrt(D * DK * TOKENS)
    flat_weight = key_weight.reshape(D, HEADS * DK)
    key_raw = jnp.dot(inputs.reshape(-1, D), flat_weight, preferred_element_type=jnp.float32)
    key_raw = key_raw.reshape(SEQS, TOKENS, HEADS, DK).astype(jnp.bfloat16)
    keys = key_raw.astype(jnp.float32) * key_scale

    def per_sequence(operands):
        query_seq, key_seq, value_seq, grad_seq = operands
        _, pullback = jax.vjp(retention, query_seq, key_seq, value_seq, decay_ahead, decay_behind)
        return pullback(grad_seq)
    grad_q, grad_k, grad_v, grad_ahead, grad_behind = lax.map(per_sequence, (queries.astype(jnp.float32), keys, values.astype(jnp.float32), out_grad.astype(jnp.float32)))
    key_grad_raw = (grad_k * key_scale).astype(jnp.bfloat16).reshape(-1, HEADS * DK)
    weight_grad = jnp.dot(inputs.reshape(-1, D).T, key_grad_raw, preferred_element_type=jnp.float32)
    weight_grad = weight_grad.reshape(D, HEADS, DK)
    input_grad = jnp.dot(key_grad_raw, flat_weight.T, preferred_element_type=jnp.float32)
    input_grad = input_grad.reshape(SEQS, TOKENS, D).astype(jnp.bfloat16)
    decay_grad = jnp.stack([lax.optimization_barrier(jnp.sum(grad_ahead, axis=0)), lax.optimization_barrier(jnp.sum(grad_behind, axis=0))])
    return (grad_q.astype(jnp.bfloat16), grad_v.astype(jnp.bfloat16), input_grad, weight_grad, decay_grad)
```

```python
import functools
import math

import jax
import jax.numpy as jnp
from jax import lax
from jax.experimental import pallas as pl
from jax.experimental.pallas import tpu as pltpu
from jax.sharding import PartitionSpec as P

F32 = jnp.float32
BF16 = jnp.bfloat16
NN = (((1,), (0,)), ((), ()))
NT = (((1,), (1,)), ((), ()))
TN = (((0,), (0,)), ((), ()))


def mm(a, b, dims):
    return lax.dot_general(a, b, dims, preferred_element_type=F32)


def kernel(
    cfg,
    rates, pack, x, w,
    gqv_out, ig_out, wg_out, dec_out,
    tok, ktok, kown, local, arrive, leave,
    kgs, kgr, gqs, gqr, dbuf, dpair, dsum, dland,
    wb, wpair, wsum, wland, isend, iland,
    tok_s, tok_r, k_s, k_r, ch_s, ch_r, kg_s, kg_r, gq_s, gq_r,
    tp_s, tp_r, pr_s, pr_r, w_s, w_r, d_s, d_r,
):
    n, tp, seqs, heads, length, dk, dv, scale = cfg
    pairs = seqs * heads
    groups = n // pairs
    half = n // 2
    chunk = pairs * length
    me = lax.axis_index("sp")
    my_tp = lax.axis_index("tp")
    group = me // pairs
    member = me % pairs
    base = group * pairs
    parity = me % 2
    mine = me // 2
    partner = me + 1 - 2 * parity
    head = member % heads

    def remote(src, dst, send, recv, device):
        return pltpu.make_async_remote_copy(
            src_ref=src, dst_ref=dst, send_sem=send, recv_sem=recv,
            device_id=device, device_id_type=pl.DeviceIdType.MESH,
        )

    barrier = pltpu.get_barrier_semaphore()
    greeted = 0
    for o in range(1, half):
        pl.semaphore_signal(
            barrier, inc=1, device_id={"sp": 2 * ((mine + o) % half) + parity},
            device_id_type=pl.DeviceIdType.MESH)
        greeted += 1
    for o in range(1, pairs, 2):
        pl.semaphore_signal(
            barrier, inc=1, device_id={"sp": base + (member + o) % pairs},
            device_id_type=pl.DeviceIdType.MESH)
        greeted += 1
    for o in range(1, tp):
        pl.semaphore_signal(
            barrier, inc=1, device_id={"tp": (my_tp + o) % tp},
            device_id_type=pl.DeviceIdType.MESH)
        greeted += 1
    pl.semaphore_wait(barrier, greeted)

    tok_copies, k_copies = [], []
    for o in range(1, pairs):
        to = (member + o) % pairs
        copy = remote(pack.at[to], tok.at[member], tok_s.at[o], tok_r.at[o], {"sp": base + to})
        copy.start()
        tok_copies.append(copy)
    key_raw = mm(x[...], w[...], NN).astype(BF16)
    for b in range(seqs):
        for h in range(heads):
            kown[b * heads + h] = key_raw[b * length:(b + 1) * length, h * dk:(h + 1) * dk]
    for o in range(1, pairs):
        to = (member + o) % pairs
        copy = remote(kown.at[to], ktok.at[member], k_s.at[o], k_r.at[o], {"sp": base + to})
        copy.start()
        k_copies.append(copy)
    tok[member] = pack[member]
    ktok[member] = kown[member]

    rate_a = rates[0, head]
    rate_b = rates[1, head]
    off = lax.broadcasted_iota(jnp.int32, (chunk, 1), 0).astype(F32)
    keep_a = jnp.exp((chunk - 1.0 - off) * rate_a)
    keep_b = jnp.exp(off * rate_b)
    reach_a = jnp.exp((off + 1.0) * rate_a)
    reach_b = jnp.exp((chunk - off) * rate_b)
    one = jnp.full((1, dv), float(chunk), F32)
    spans = (jnp.exp(one * rate_a), jnp.exp(one * rate_b))

    for copy in tok_copies:
        copy.wait_recv()
    q = tok[:, :, :dk].reshape(chunk, dk)
    v = tok[:, :, dk:dk + dv].reshape(chunk, dv)
    do = tok[:, :, dk + dv:].reshape(chunk, dv)
    qf = q.astype(F32)
    local[0, 1] = mm((qf * reach_b).astype(BF16), do, TN)
    local[1, 0] = mm((qf * reach_a).astype(BF16), do, TN)
    for copy in k_copies:
        copy.wait_recv()
    k = ktok[...].reshape(chunk, dk)
    kf = k.astype(F32)
    local[0, 0] = mm((kf * keep_a).astype(BF16), v, TN)
    local[1, 1] = mm((kf * keep_b).astype(BF16), v, TN)

    low = group < (groups + 1) // 2

    def chain(j):
        way = jnp.where(low, j, 1 - j)
        has_in = jnp.where(way == 0, group > 0, group < groups - 1)
        has_out = jnp.where(way == 0, group < groups - 1, group > 0)
        nxt = jnp.clip(group + 1 - 2 * way, 0, groups - 1) * pairs + member
        for kind in range(2):
            copy = remote(leave.at[way, kind], arrive.at[way, kind], ch_s.at[way, kind],
                          ch_r.at[way, kind], {"sp": nxt})

            @pl.when(has_in)
            def _():
                copy.wait_recv()

            @pl.when(jnp.logical_not(has_in))
            def _():
                arrive[way, kind] = jnp.zeros(arrive.shape[2:], BF16)

            @pl.when(has_out)
            def _():
                leave[way, kind] = (
                    spans[kind] * arrive[way, kind].astype(F32) + local[way, kind]
                ).astype(BF16)
                copy.start()

    def chain_end(j):
        way = jnp.where(low, j, 1 - j)
        has_out = jnp.where(way == 0, group < groups - 1, group > 0)
        nxt = jnp.clip(group + 1 - 2 * way, 0, groups - 1) * pairs + member
        for kind in range(2):
            copy = remote(leave.at[way, kind], arrive.at[way, kind], ch_s.at[way, kind],
                          ch_r.at[way, kind], {"sp": nxt})

            @pl.when(has_out)
            def _():
                copy.wait_send()

    chain(0)
    scores = mm(q, k, NT) * scale
    grads = mm(do, v, NT)
    dist = (lax.broadcasted_iota(jnp.int32, (chunk, chunk), 0)
            - lax.broadcasted_iota(jnp.int32, (chunk, chunk), 1)).astype(F32)
    gap = jnp.abs(dist)
    decay = jnp.exp(gap * jnp.where(dist >= 0, rate_a, rate_b))
    mask = jnp.where(dist == 0, 2.0, decay)
    gm = grads * mask
    weighted = gm * scores * gap
    in_a = jnp.sum(jnp.where(dist > 0, weighted, 0.0))
    in_b = jnp.sum(jnp.where(dist < 0, weighted, 0.0))
    gm = gm.astype(BF16)
    sm = (scores * mask).astype(BF16)
    grad_q = mm(gm, k, NN)
    grad_k = mm(gm, q, TN)
    grad_v = mm(sm, do, TN)
    chain(1)

    ka = keep_a * mm(v, arrive[1, 0], NT)
    kb = keep_b * mm(v, arrive[0, 1], NT)
    kgs[...] = ((grad_k + ka + kb) * scale).astype(BF16).reshape(pairs, length, dk)
    kg_copies = []
    for o in range(1, pairs):
        to = (member + o) % pairs
        copy = remote(kgs.at[to], kgr.at[member], kg_s.at[o], kg_r.at[o], {"sp": base + to})
        copy.start()
        kg_copies.append(copy)
    kgr[member] = kgs[member]
    qa = reach_a * mm(do, arrive[0, 0], NT)
    qb = reach_b * mm(do, arrive[1, 1], NT)
    gqs[:, :, :dk] = ((grad_q + qa + qb) * scale).astype(BF16).reshape(pairs, length, dk)
    far_v = keep_a * mm(k, arrive[1, 0], NN) + keep_b * mm(k, arrive[0, 1], NN)
    gqs[:, :, dk:] = (grad_v + far_v * scale).astype(BF16).reshape(pairs, length, dv)
    gq_copies = []
    for o in range(1, pairs):
        to = (member + o) % pairs
        copy = remote(gqs.at[to], gqr.at[member], gq_s.at[o], gq_r.at[o], {"sp": base + to})
        copy.start()
        gq_copies.append(copy)
    gqr[member] = gqs[member]
    pos = off + ((group * chunk).astype(F32) - 0.5 * (chunk * groups))
    sum_a = in_a + scale * jnp.sum(pos * (qf * qa - kf * ka))
    sum_b = in_b + scale * jnp.sum(pos * (kf * kb - qf * qb))
    row = lax.broadcasted_iota(jnp.int32, dbuf.shape, 0)
    lane = lax.broadcasted_iota(jnp.int32, dbuf.shape, 1)
    dbuf[...] = jnp.where(lane == head, jnp.where(row == 0, sum_a, jnp.where(row == 1, sum_b, 0.0)), 0.0)
    d_pair = remote(dbuf, dpair, pr_s.at[1], pr_r.at[1], {"sp": partner})
    d_pair.start()

    for copy in kg_copies:
        copy.wait_recv()
    own_seqs = seqs // tp
    tp_copies = []

    def seq_rows(b):
        return jnp.concatenate([kgr[b * heads + h] for h in range(heads)], axis=1)

    for o in range(1, tp):
        to = (my_tp + o) % tp
        for s in range(own_seqs):
            isend[o - 1, s * length:(s + 1) * length] = mm(
                seq_rows(to * own_seqs + s), w[...], NT).astype(BF16)
        copy = remote(isend.at[o - 1], iland.at[o - 1], tp_s.at[o - 1], tp_r.at[o - 1], {"tp": to})
        copy.start()
        tp_copies.append(copy)
    kg_all = jnp.concatenate([seq_rows(b) for b in range(seqs)], axis=0)
    wp = mm(x[...], kg_all, TN).astype(BF16).reshape(half, 2, -1, heads * dk)
    wb[0] = wp[:, 0]
    wb[1] = wp[:, 1]
    w_pair = remote(wb.at[1 - parity], wpair, pr_s.at[0], pr_r.at[0], {"sp": partner})
    w_pair.start()
    d_pair.wait_recv()
    dsum[...] = dbuf[...] + dpair[...]
    w_copies, d_copies = [], []
    for o in range(1, half):
        to = 2 * ((mine + o) % half) + parity
        copy = remote(dsum, dland.at[o - 1], d_s.at[o - 1], d_r.at[o - 1], {"sp": to})
        copy.start()
        d_copies.append(copy)
    own_ig = [mm(seq_rows(my_tp * own_seqs + s), w[...], NT) for s in range(own_seqs)]
    w_pair.wait_recv()
    wsum[...] = (wb[parity].astype(F32) + wpair[...].astype(F32)).astype(BF16)
    for o in range(1, half):
        j = (mine + o) % half
        copy = remote(wsum.at[j], wland.at[o - 1], w_s.at[o - 1], w_r.at[o - 1],
                      {"sp": 2 * j + parity})
        copy.start()
        w_copies.append(copy)
    for copy in gq_copies:
        copy.wait_recv()
    gqv_out[...] = gqr[...]
    for copy in tp_copies:
        copy.wait_recv()
    for s in range(own_seqs):
        total = own_ig[s]
        for o in range(tp - 1):
            total = total + iland[o, s * length:(s + 1) * length].astype(F32)
        ig_out[s * length:(s + 1) * length] = total.astype(BF16)
    total = dsum[...]
    for o, copy in enumerate(d_copies):
        copy.wait_recv()
        total = total + dland[o]
    dec_out[...] = total
    total = wsum[mine].astype(F32)
    for o, copy in enumerate(w_copies):
        copy.wait_recv()
        total = total + wland[o].astype(F32)
    wg_out[...] = total
    chain_end(0)
    chain_end(1)
    for copy in (tok_copies + k_copies + kg_copies + gq_copies + tp_copies + w_copies + d_copies
                 + [d_pair, w_pair]):
        copy.wait_send()


def shards(n, tp, inputs, queries, values, out_grad, key_weight, decay_ahead, decay_behind):
    seqs, length, width = inputs.shape
    heads, dk, dv = queries.shape[2], queries.shape[3], values.shape[3]
    pairs = seqs * heads
    all_tokens = length * n
    scale = 1.0 / math.sqrt(width * dk * all_tokens)
    decays = jnp.stack([decay_ahead, decay_behind])
    rates = jax.nn.log_sigmoid(decays) / all_tokens
    pack = jnp.concatenate([queries, values, out_grad], axis=3)
    pack = pack.transpose(0, 2, 1, 3).reshape(pairs, length, dk + 2 * dv)
    x = inputs.reshape(seqs * length, width)
    w = key_weight.reshape(width, heads * dk)
    half, rows, own = n // 2, width // n, seqs // tp
    vm = pl.BlockSpec(memory_space=pltpu.VMEM)
    dma = pltpu.SemaphoreType.DMA
    gqv, ig, wg, dec = pl.pallas_call(
        functools.partial(kernel, (n, tp, seqs, heads, length, dk, dv, scale)),
        out_shape=(
            jax.ShapeDtypeStruct((pairs, length, dk + dv), BF16),
            jax.ShapeDtypeStruct((own * length, width), BF16),
            jax.ShapeDtypeStruct((rows, heads * dk), F32),
            jax.ShapeDtypeStruct((8, 128), F32),
        ),
        in_specs=[pl.BlockSpec(memory_space=pltpu.SMEM), vm, vm, vm],
        out_specs=(vm, vm, vm, vm),
        scratch_shapes=[
            pltpu.VMEM((pairs, length, dk + 2 * dv), BF16),
            pltpu.VMEM((pairs, length, dk), BF16),
            pltpu.VMEM((pairs, length, dk), BF16),
            pltpu.VMEM((2, 2, dk, dv), F32),
            pltpu.VMEM((2, 2, dk, dv), BF16),
            pltpu.VMEM((2, 2, dk, dv), BF16),
            pltpu.VMEM((pairs, length, dk), BF16),
            pltpu.VMEM((pairs, length, dk), BF16),
            pltpu.VMEM((pairs, length, dk + dv), BF16),
            pltpu.VMEM((pairs, length, dk + dv), BF16),
            pltpu.VMEM((8, 128), F32),
            pltpu.VMEM((8, 128), F32),
            pltpu.VMEM((8, 128), F32),
            pltpu.VMEM((half - 1, 8, 128), F32),
            pltpu.VMEM((2, half, rows, heads * dk), BF16),
            pltpu.VMEM((half, rows, heads * dk), BF16),
            pltpu.VMEM((half, rows, heads * dk), BF16),
            pltpu.VMEM((half - 1, rows, heads * dk), BF16),
            pltpu.VMEM((tp - 1, own * length, width), BF16),
            pltpu.VMEM((tp - 1, own * length, width), BF16),
            dma((pairs,)), dma((pairs,)), dma((pairs,)), dma((pairs,)),
            dma((2, 2)), dma((2, 2)),
            dma((pairs,)), dma((pairs,)), dma((pairs,)), dma((pairs,)),
            dma((tp - 1,)), dma((tp - 1,)), dma((2,)), dma((2,)),
            dma((half - 1,)), dma((half - 1,)), dma((half - 1,)), dma((half - 1,)),
        ],
        compiler_params=pltpu.CompilerParams(
            collective_id=0, has_side_effects=True, vmem_limit_bytes=50 * 1024 * 1024
        ),
    )(rates, pack, x, w)
    gqv = gqv.reshape(seqs, heads, length, dk + dv).transpose(0, 2, 1, 3)
    slopes = jax.nn.sigmoid(-decays) / all_tokens
    return (
        gqv[..., :dk],
        gqv[..., dk:],
        ig.reshape(own, length, width),
        wg.reshape(rows, heads, dk),
        dec[:2, :heads] * slopes,
    )


def solution(mesh):
    in_specs = (
        P(None, "sp", None),
        P(None, "sp", "tp", None),
        P(None, "sp", "tp", None),
        P(None, "sp", "tp", None),
        P(None, "tp", None),
        P("tp"),
        P("tp"),
    )
    out_specs = (
        P(None, "sp", "tp", None),
        P(None, "sp", "tp", None),
        P("tp", "sp", None),
        P("sp", "tp", None),
        P(None, "tp"),
    )
    body = functools.partial(shards, mesh.shape["sp"], mesh.shape["tp"])
    return jax.shard_map(body, mesh=mesh, in_specs=in_specs, out_specs=out_specs, check_vma=False)
```

```python
import functools
import math

import jax
import jax.numpy as jnp
from jax import lax
from jax.experimental import pallas as pl
from jax.experimental.pallas import tpu as pltpu
from jax.sharding import PartitionSpec as P

F32 = jnp.float32
BF16 = jnp.bfloat16
NN = (((1,), (0,)), ((), ()))
NT = (((1,), (1,)), ((), ()))
TN = (((0,), (0,)), ((), ()))


def mm(a, b, dims):
    return lax.dot_general(a, b, dims, preferred_element_type=F32)


def kernel(
    cfg,
    ahead, behind, pack, x, w,
    q_out, v_out, ig_out, wg_out, dec_out,
    xt, mask, gm, tok, ktok, kown, local, arrive, leave,
    kgs, kgr, gqs, gqr, dbuf, dpair, dsum, dland,
    wb, wpair, wsum, wland, isend, iland,
    tok_s, tok_r, v_s, v_r, k_s, k_r, ch_s, ch_r, kg_s, kg_r, gq_s, gq_r,
    tp_s, tp_r, pr_s, pr_r, w_s, w_r, d_s, d_r,
):
    n, tp, seqs, heads, length, dk, dv, scale = cfg
    pairs = seqs * heads
    groups = n // pairs
    half = n // 2
    chunk = pairs * length
    me = lax.axis_index("sp")
    my_tp = lax.axis_index("tp")
    group = me // pairs
    member = me % pairs
    base = group * pairs
    parity = me % 2
    mine = me // 2
    partner = me + 1 - 2 * parity
    head = member % heads

    def remote(src, dst, send, recv, device):
        return pltpu.make_async_remote_copy(
            src_ref=src, dst_ref=dst, send_sem=send, recv_sem=recv,
            device_id=device, device_id_type=pl.DeviceIdType.MESH,
        )

    barrier = pltpu.get_barrier_semaphore()
    greeted = 0
    for o in range(1, half):
        pl.semaphore_signal(
            barrier, inc=1, device_id={"sp": 2 * ((mine + o) % half) + parity},
            device_id_type=pl.DeviceIdType.MESH)
        greeted += 1
    for o in range(1, pairs, 2):
        pl.semaphore_signal(
            barrier, inc=1, device_id={"sp": base + (member + o) % pairs},
            device_id_type=pl.DeviceIdType.MESH)
        greeted += 1
    for o in range(1, tp):
        pl.semaphore_signal(
            barrier, inc=1, device_id={"tp": (my_tp + o) % tp},
            device_id_type=pl.DeviceIdType.MESH)
        greeted += 1
    pl.semaphore_wait(barrier, greeted)

    early = dk + dv
    tok_copies, v_copies, k_copies = [], [], []
    for o in range(1, pairs):
        to = (member + o) % pairs
        copy = remote(pack.at[to, :, pl.ds(0, early)], tok.at[member, :, pl.ds(0, early)],
                      tok_s.at[o], tok_r.at[o], {"sp": base + to})
        copy.start()
        tok_copies.append(copy)
    for o in range(1, pairs):
        to = (member + o) % pairs
        copy = remote(pack.at[to, :, pl.ds(early, dv)], tok.at[member, :, pl.ds(early, dv)],
                      v_s.at[o], v_r.at[o], {"sp": base + to})
        copy.start()
        v_copies.append(copy)
    key_raw = mm(x[...], w[...], NN).astype(BF16)
    for b in range(seqs):
        for h in range(heads):
            kown[b * heads + h] = key_raw[b * length:(b + 1) * length, h * dk:(h + 1) * dk]
    for o in range(1, pairs):
        to = (member + o) % pairs
        copy = remote(kown.at[to], ktok.at[member], k_s.at[o], k_r.at[o], {"sp": base + to})
        copy.start()
        k_copies.append(copy)
    tok[member] = pack[member]
    ktok[member] = kown[member]

    def rate_and_slope(ref):
        raw = jnp.full((1, 1), ref[head], F32)
        rate = jnp.minimum(raw, 0.0) - jnp.log(1.0 + jnp.exp(-jnp.abs(raw)))
        return rate / (length * n), 1.0 / ((1.0 + jnp.exp(raw)) * (length * n))

    rate_a, slope_a = rate_and_slope(ahead)
    rate_b, slope_b = rate_and_slope(behind)
    off = lax.broadcasted_iota(jnp.int32, (chunk, 1), 0).astype(F32)
    keep_a = jnp.exp((chunk - 1.0 - off) * rate_a)
    keep_b = jnp.exp(off * rate_b)
    reach_a = jnp.exp((off + 1.0) * rate_a)
    reach_b = jnp.exp((chunk - off) * rate_b)
    span_a = jnp.exp(chunk * rate_a)
    span_b = jnp.exp(chunk * rate_b)
    dist = (lax.broadcasted_iota(jnp.int32, (chunk, chunk), 0)
            - lax.broadcasted_iota(jnp.int32, (chunk, chunk), 1)).astype(F32)
    decay = jnp.exp(jnp.abs(dist) * jnp.where(dist >= 0, rate_a, rate_b))
    mask[...] = jnp.where(dist == 0, 2.0, decay)
    xt[...] = x[...].T

    low = group < (groups + 1) // 2
    piece = dk // 2

    def chain(j, pull, finish=False):
        way = jnp.where(low, j, 1 - j)
        kind = 1 - way if pull else way
        span = jnp.where(kind == 0, span_a, span_b)
        has_in = jnp.where(way == 0, group > 0, group < groups - 1)
        has_out = jnp.where(way == 0, group < groups - 1, group > 0)
        nxt = jnp.clip(group + 1 - 2 * way, 0, groups - 1) * pairs + member
        for c in range(2):
            rows = pl.ds(c * piece, piece)
            copy = remote(leave.at[way, kind, rows], arrive.at[way, kind, rows],
                          ch_s.at[way, kind, c], ch_r.at[way, kind, c], {"sp": nxt})
            if finish:
                @pl.when(has_out)
                def _():
                    copy.wait_send()
                continue

            @pl.when(has_in)
            def _():
                copy.wait_recv()

            @pl.when(jnp.logical_not(has_in))
            def _():
                arrive[way, kind, rows] = jnp.zeros((piece, dv), BF16)

            @pl.when(has_out)
            def _():
                leave[way, kind, rows] = (
                    span * arrive[way, kind, rows].astype(F32) + local[way, kind, rows]
                ).astype(BF16)
                copy.start()

    for copy in tok_copies:
        copy.wait_recv()
    q = tok[:, :, :dk].reshape(chunk, dk)
    do = tok[:, :, dk:early].reshape(chunk, dv)
    qf = q.astype(F32)
    local[0, 1] = mm((qf * reach_b).astype(BF16), do, TN)
    local[1, 0] = mm((qf * reach_a).astype(BF16), do, TN)
    chain(0, True)
    for copy in v_copies:
        copy.wait_recv()
    v = tok[:, :, early:].reshape(chunk, dv)
    gm[...] = mm(do, v, NT) * mask[...]
    for copy in k_copies:
        copy.wait_recv()
    k = ktok[...].reshape(chunk, dk)
    kf = k.astype(F32)
    local[0, 0] = mm((kf * keep_a).astype(BF16), v, TN)
    local[1, 1] = mm((kf * keep_b).astype(BF16), v, TN)
    chain(0, False)
    chain(1, True)
    sm = mm(q, k, NT) * scale
    weighted = gm[...] * sm
    in_a = jnp.sum(weighted * jnp.maximum(dist, 0.0))
    in_b = jnp.sum(weighted * jnp.maximum(-dist, 0.0))
    sm = (sm * mask[...]).astype(BF16)
    gmb = gm[...].astype(BF16)
    grad_q = mm(gmb, k, NN)
    grad_k = mm(gmb, q, TN)
    grad_v = mm(sm, do, TN)
    chain(1, False)

    ka = keep_a * mm(v, arrive[1, 0], NT)
    kb = keep_b * mm(v, arrive[0, 1], NT)
    kgs[...] = ((grad_k + ka + kb) * scale).astype(BF16).reshape(pairs, length, dk)
    kg_copies = []
    for o in range(1, pairs):
        to = (member + o) % pairs
        copy = remote(kgs.at[to], kgr.at[member], kg_s.at[o], kg_r.at[o], {"sp": base + to})
        copy.start()
        kg_copies.append(copy)
    kgr[member] = kgs[member]
    qa = reach_a * mm(do, arrive[0, 0], NT)
    qb = reach_b * mm(do, arrive[1, 1], NT)
    gqs[:, :, :dk] = ((grad_q + qa + qb) * scale).astype(BF16).reshape(pairs, length, dk)
    far_v = keep_a * mm(k, arrive[1, 0], NN) + keep_b * mm(k, arrive[0, 1], NN)
    gqs[:, :, dk:] = (grad_v + far_v * scale).astype(BF16).reshape(pairs, length, dv)
    gq_copies = []
    for o in range(1, pairs):
        to = (member + o) % pairs
        copy = remote(gqs.at[to], gqr.at[member], gq_s.at[o], gq_r.at[o], {"sp": base + to})
        copy.start()
        gq_copies.append(copy)
    gqr[member] = gqs[member]
    pos = off + ((group * chunk).astype(F32) - 0.5 * (chunk * groups))
    sum_a = slope_a * (in_a + scale * jnp.sum(pos * (qf * qa - kf * ka)))
    sum_b = slope_b * (in_b + scale * jnp.sum(pos * (kf * kb - qf * qb)))
    row = lax.broadcasted_iota(jnp.int32, dbuf.shape, 0)
    lane = lax.broadcasted_iota(jnp.int32, dbuf.shape, 1)
    dbuf[...] = jnp.where(lane == head, jnp.where(row == 0, sum_a, jnp.where(row == 1, sum_b, 0.0)), 0.0)
    d_pair = remote(dbuf, dpair, pr_s.at[1], pr_r.at[1], {"sp": partner})
    d_pair.start()

    for copy in kg_copies:
        copy.wait_recv()
    own_seqs = seqs // tp
    tp_copies = []

    def seq_rows(b):
        return jnp.concatenate([kgr[b * heads + h] for h in range(heads)], axis=1)

    for o in range(1, tp):
        to = (my_tp + o) % tp
        for s in range(own_seqs):
            isend[o - 1, s * length:(s + 1) * length] = mm(
                seq_rows(to * own_seqs + s), w[...], NT).astype(BF16)
        copy = remote(isend.at[o - 1], iland.at[o - 1], tp_s.at[o - 1], tp_r.at[o - 1], {"tp": to})
        copy.start()
        tp_copies.append(copy)
    kg_all = jnp.concatenate([seq_rows(b) for b in range(seqs)], axis=0)
    wp = mm(xt[...], kg_all, NN).astype(BF16).reshape(half, 2, -1, heads * dk)
    wb[0] = wp[:, 0]
    wb[1] = wp[:, 1]
    w_pair = remote(wb.at[1 - parity], wpair, pr_s.at[0], pr_r.at[0], {"sp": partner})
    w_pair.start()
    d_pair.wait_recv()
    dsum[...] = dbuf[...] + dpair[...]
    w_copies, d_copies = [], []
    for o in range(1, half):
        to = 2 * ((mine + o) % half) + parity
        copy = remote(dsum, dland.at[o - 1], d_s.at[o - 1], d_r.at[o - 1], {"sp": to})
        copy.start()
        d_copies.append(copy)
    own_ig = [mm(seq_rows(my_tp * own_seqs + s), w[...], NT) for s in range(own_seqs)]
    w_pair.wait_recv()
    wsum[...] = (wb[parity].astype(F32) + wpair[...].astype(F32)).astype(BF16)
    for o in range(1, half):
        j = (mine + o) % half
        copy = remote(wsum.at[j], wland.at[o - 1], w_s.at[o - 1], w_r.at[o - 1],
                      {"sp": 2 * j + parity})
        copy.start()
        w_copies.append(copy)
    for copy in gq_copies:
        copy.wait_recv()
    q_out[...] = gqr[:, :, :dk]
    v_out[...] = gqr[:, :, dk:]
    for copy in tp_copies:
        copy.wait_recv()
    for s in range(own_seqs):
        total = own_ig[s]
        for o in range(tp - 1):
            total = total + iland[o, s * length:(s + 1) * length].astype(F32)
        ig_out[s * length:(s + 1) * length] = total.astype(BF16)
    total = dsum[...]
    for o, copy in enumerate(d_copies):
        copy.wait_recv()
        total = total + dland[o]
    dec_out[...] = total
    total = wsum[mine].astype(F32)
    for o, copy in enumerate(w_copies):
        copy.wait_recv()
        total = total + wland[o].astype(F32)
    wg_out[...] = total
    for j in range(2):
        chain(j, True, True)
        chain(j, False, True)
    for copy in (tok_copies + v_copies + k_copies + kg_copies + gq_copies + tp_copies + w_copies + d_copies
                 + [d_pair, w_pair]):
        copy.wait_send()


def shards(n, tp, inputs, queries, values, out_grad, key_weight, decay_ahead, decay_behind):
    seqs, length, width = inputs.shape
    heads, dk, dv = queries.shape[2], queries.shape[3], values.shape[3]
    pairs = seqs * heads
    all_tokens = length * n
    scale = 1.0 / math.sqrt(width * dk * all_tokens)
    pack = jnp.concatenate([queries, out_grad, values], axis=3)
    pack = pack.transpose(0, 2, 1, 3).reshape(pairs, length, dk + 2 * dv)
    x = inputs.reshape(seqs * length, width)
    w = key_weight.reshape(width, heads * dk)
    half, rows, own = n // 2, width // n, seqs // tp
    vm = pl.BlockSpec(memory_space=pltpu.VMEM)
    sm = pl.BlockSpec(memory_space=pltpu.SMEM)
    chunk = pairs * length
    dma = pltpu.SemaphoreType.DMA
    gq, gv, ig, wg, dec = pl.pallas_call(
        functools.partial(kernel, (n, tp, seqs, heads, length, dk, dv, scale)),
        out_shape=(
            jax.ShapeDtypeStruct((pairs, length, dk), BF16),
            jax.ShapeDtypeStruct((pairs, length, dv), BF16),
            jax.ShapeDtypeStruct((own * length, width), BF16),
            jax.ShapeDtypeStruct((rows, heads * dk), F32),
            jax.ShapeDtypeStruct((8, 128), F32),
        ),
        in_specs=[sm, sm, vm, vm, vm],
        out_specs=(vm, vm, vm, vm, vm),
        scratch_shapes=[
            pltpu.VMEM((width, seqs * length), BF16),
            pltpu.VMEM((chunk, chunk), F32),
            pltpu.VMEM((chunk, chunk), F32),
            pltpu.VMEM((pairs, length, dk + 2 * dv), BF16),
            pltpu.VMEM((pairs, length, dk), BF16),
            pltpu.VMEM((pairs, length, dk), BF16),
            pltpu.VMEM((2, 2, dk, dv), F32),
            pltpu.VMEM((2, 2, dk, dv), BF16),
            pltpu.VMEM((2, 2, dk, dv), BF16),
            pltpu.VMEM((pairs, length, dk), BF16),
            pltpu.VMEM((pairs, length, dk), BF16),
            pltpu.VMEM((pairs, length, dk + dv), BF16),
            pltpu.VMEM((pairs, length, dk + dv), BF16),
            pltpu.VMEM((8, 128), F32),
            pltpu.VMEM((8, 128), F32),
            pltpu.VMEM((8, 128), F32),
            pltpu.VMEM((half - 1, 8, 128), F32),
            pltpu.VMEM((2, half, rows, heads * dk), BF16),
            pltpu.VMEM((half, rows, heads * dk), BF16),
            pltpu.VMEM((half, rows, heads * dk), BF16),
            pltpu.VMEM((half - 1, rows, heads * dk), BF16),
            pltpu.VMEM((tp - 1, own * length, width), BF16),
            pltpu.VMEM((tp - 1, own * length, width), BF16),
            dma((pairs,)), dma((pairs,)), dma((pairs,)), dma((pairs,)),
            dma((pairs,)), dma((pairs,)),
            dma((2, 2, 2)), dma((2, 2, 2)),
            dma((pairs,)), dma((pairs,)), dma((pairs,)), dma((pairs,)),
            dma((tp - 1,)), dma((tp - 1,)), dma((2,)), dma((2,)),
            dma((half - 1,)), dma((half - 1,)), dma((half - 1,)), dma((half - 1,)),
        ],
        compiler_params=pltpu.CompilerParams(
            collective_id=0, has_side_effects=True, vmem_limit_bytes=50 * 1024 * 1024
        ),
    )(decay_ahead, decay_behind, pack, x, w)

    def tokens_first(grad):
        return grad.reshape(seqs, heads, length, -1).transpose(0, 2, 1, 3)

    return (
        tokens_first(gq),
        tokens_first(gv),
        ig.reshape(own, length, width),
        wg.reshape(rows, heads, dk),
        dec[:2, :heads],
    )


def solution(mesh):
    in_specs = (
        P(None, "sp", None),
        P(None, "sp", "tp", None),
        P(None, "sp", "tp", None),
        P(None, "sp", "tp", None),
        P(None, "tp", None),
        P("tp"),
        P("tp"),
    )
    out_specs = (
        P(None, "sp", "tp", None),
        P(None, "sp", "tp", None),
        P("tp", "sp", None),
        P("sp", "tp", None),
        P(None, "tp"),
    )
    body = functools.partial(shards, mesh.shape["sp"], mesh.shape["tp"])
    return jax.shard_map(body, mesh=mesh, in_specs=in_specs, out_specs=out_specs, check_vma=False)
```
